32 devices in a mesh: ra: 4 (over y, x), cb: 8 (over z, core).
Axes of the slice: x: 2, y: 2, z: 4, core: 2. Of those that a mesh axis runs over, the one named last changes fastest.
Arguments:
- tokens: bfloat16 [256, 4096], P(None, 'ra'), may hold values from -20 to 20, as said below
- norm_gain: float32 [2, 4096], P(None, 'ra'), may hold values from 0.1 to 1.9
- gate_weight: bfloat16 [2, 4096, 11008], P(None, 'ra', 'cb'), may hold values from -0.09375 to 0.09375
- value_weight: bfloat16 [2, 4096, 11008], P(None, 'ra', 'cb'), may hold values from -0.09375 to 0.09375
- gate_taps: float32 [2, 3, 11008], P(None, None, 'cb'), may hold values from -3.5 to 3.5
- value_taps: float32 [2, 3, 11008], P(None, None, 'cb'), may hold values from -3.5 to 3.5
- down_weight: bfloat16 [2, 11008, 4096], P(None, 'cb', 'ra'), may hold values from -0.0546875 to 0.0546875
Outputs:
- mixed: bfloat16 [256, 4096], P(None, 'ra')
The draws below stay inside these ranges and needn't reach their ends.
Inputs may be any that keep to these rules, and one draw needn't show every extreme that they name: tokens have features drawn around zero with a scale that varies by blocks of features between about 0.3 and 3.3.
All inputs are finite; a program needn't handle non-finite values.
Results may differ from the reference program's by a relative error of at most 0.0075.
Values may be sent and summed in bfloat16 or wider, within the bound.
A program may use at most 128 MiB of HBM per device.

```python
import jax
import jax.numpy as jnp
from jax import lax

D = 4096
FF = 11008
KERNEL = 3
LAYERS = 2
TOKENS = 256


def draw_tokens(key, part):
    base_key, scale_key = jax.random.split(jax.random.fold_in(key, 11))
    block_scales = jnp.exp(jax.random.uniform(scale_key, (64,), jnp.float32, -1.2, 1.2))
    column_scales = jnp.repeat(block_scales, D // 64)
    base = jnp.clip(jax.random.normal(base_key, (TOKENS, D), jnp.float32), -6.0, 6.0)
    return (base * column_scales[None, :]).astype(jnp.bfloat16)


def block_levels(stream_key, shape, pieces, least, top_value):
    factor_of = 1.0
    for position, blocks in pieces:
        draws = jax.random.uniform(jax.random.fold_in(jax.random.fold_in(stream_key, 6), position), (blocks,), jnp.float32, least / len(pieces), top_value / len(pieces))
        factor_of = factor_of * jnp.repeat(jnp.exp(draws), shape[position] // blocks).reshape((-1,) + (1,) * (len(shape) - 1 - position))
    return factor_of


def bell_draw(stream_key, dims, spread, most, shards=(), held_as=jnp.bfloat16):
    drawn = spread * jax.random.normal(stream_key, dims, jnp.float32)
    if shards:
        drawn = drawn * block_levels(stream_key, dims, shards, -0.22, 0.18)
    return jnp.clip(drawn, -most, most).astype(held_as)


def setup_inputs(seed: int = 0) -> dict:
    keys = jax.random.split(jax.random.key(seed), 8)
    return {
        "tokens": draw_tokens(jax.random.fold_in(keys[7], 71), 0),
        "norm_gain": jnp.clip(1.0 + 0.18 * jax.random.normal(keys[1], (LAYERS, D), jnp.float32), 0.1, 1.9),
        "gate_weight": bell_draw(keys[2], (LAYERS, D, FF), D ** -0.5, 0.09375, ((1, 4), (2, 8))),
        "value_weight": bell_draw(keys[3], (LAYERS, D, FF), D ** -0.5, 0.09375, ((1, 4), (2, 8))),
        "gate_taps": bell_draw(keys[4], (LAYERS, KERNEL, FF), KERNEL ** -0.5, 3.5, ((2, 8),), jnp.float32),
        "value_taps": bell_draw(keys[5], (LAYERS, KERNEL, FF), KERNEL ** -0.5, 3.5, ((2, 8),), jnp.float32),
        "down_weight": bell_draw(keys[6], (LAYERS, FF, D), FF ** -0.5, 0.0546875, ((1, 8), (2, 4))),
    }


epsilon = 1e-06

def causal_conv(signal, kernel_taps):
    length = signal.shape[0]
    width = kernel_taps.shape[0]
    padded = jnp.concatenate([jnp.zeros((width - 1, signal.shape[1]), jnp.float32), signal], axis=0)
    result = jnp.zeros(signal.shape, jnp.float32)
    for offset in range(width):
        result = result + kernel_taps[offset] * padded[offset:offset + length]
    return result

def reference(tokens, norm_gain, gate_weight, value_weight, gate_taps, value_taps, down_weight):
    stream = tokens
    for layer_index in range(LAYERS):
        current = stream.astype(jnp.float32)
        inverse_rms = lax.rsqrt(lax.optimization_barrier(jnp.sum(current * current, axis=1, keepdims=True)) / D + epsilon)
        scaled = (current * norm_gain[layer_index]).astype(jnp.bfloat16)
        gate_lin = jnp.dot(scaled, gate_weight[layer_index], preferred_element_type=jnp.float32) * inverse_rms
        value_lin = jnp.dot(scaled, value_weight[layer_index], preferred_element_type=jnp.float32) * inverse_rms
        gate_conv = causal_conv(gate_lin, gate_taps[layer_index])
        value_conv = causal_conv(value_lin, value_taps[layer_index])
        hidden = (jax.nn.silu(gate_conv) * value_conv).astype(jnp.bfloat16)
        branch = jnp.dot(hidden, down_weight[layer_index], preferred_element_type=jnp.float32)
        stream = (0.5 * current + branch).astype(jnp.bfloat16)
    return stream
```

```python
import functools

import jax
import jax.numpy as jnp
from jax import lax
from jax.experimental import pallas as pl
from jax.experimental.pallas import tpu as pltpu
from jax.sharding import PartitionSpec as P

epsilon = 1e-06
MESH = pl.DeviceIdType.MESH
CORES = 2


def lane_tiles(width, tile=512):
    return [(start, min(tile, width - start)) for start in range(0, width, tile)]


def schedule(layers, chunks):
    order = []
    for layer in range(layers):
        if chunks == 1:
            order += [(s, layer, 0) for s in ("ua", "ub", "h", "wa", "wb", "sa", "sb", "sc")]
            continue
        for c in range(chunks):
            order += [("sc", layer - 1, c)] if layer else []
            order += [("ua", layer, c), ("ub", layer, c)]
        for c in range(chunks):
            order += [("h", layer, c)]
            if c:
                order += [("wb", layer, c - 1)]
            order += [("wa", layer, c)]
            if c:
                order += [("sa", layer, c - 1)]
        order += [("wb", layer, chunks - 1)]
        for c in range(chunks - 1):
            order += [("sb", layer, c)]
        order += [("sa", layer, chunks - 1), ("sb", layer, chunks - 1)]
    if chunks > 1:
        order += [("sc", layers - 1, c) for c in range(chunks)]
    return order


def kernel(
    cfg,
    tokens, gain, gate_hbm, value_hbm, gate_taps, value_taps, down_hbm,
    out,
    wg, wv, wd, buf, sums_out, sums_in, part, part_in, hid, acc, half, half_in, red, red_in, strm,
    w_sem, sums_ss, sums_rs, part_ss, part_rs, hid_ss, hid_rs, half_ss, half_rs, red_ss, red_rs,
    strm_ss, strm_rs, pair_ss, pair_rs,
):
    layers, chunks, nr, nz, t, ff, d, total_d = cfg
    tr = t // nr
    tz = t // (CORES * nz)
    r = lax.axis_index("ra")
    cb = lax.axis_index("cb")
    z, k = cb // CORES, lax.rem(cb, CORES)
    pair = (r, z * CORES + 1 - k)

    def ra_peer(off):
        return lax.rem(r + off, nr)

    def z_peer(off):
        return lax.rem(z + off, nz)

    def weight_copies(layer):
        return [
            pltpu.make_async_copy(src.at[layer], dst.at[layer], w_sem.at[layer, i])
            for i, (src, dst) in enumerate(((gate_hbm, wg), (value_hbm, wv), (down_hbm, wd)))
        ]

    weights = [weight_copies(layer) for layer in range(layers)]
    for copies in weights:
        for copy in copies:
            copy.start()

    barrier = pltpu.get_barrier_semaphore()
    peers = [(ra_peer(o), cb) for o in range(1, nr)]
    peers += [(r, z_peer(o) * CORES + k) for o in range(1, nz)] + [pair]
    for peer in peers:
        pl.semaphore_signal(barrier, inc=1, device_id=peer, device_id_type=MESH)
    pl.semaphore_wait(barrier, len(peers))

    pending = []

    def send(src, dst, ssem, rsem, device):
        copy = pltpu.make_async_remote_copy(
            src_ref=src, dst_ref=dst, send_sem=ssem, recv_sem=rsem,
            device_id=device, device_id_type=MESH,
        )
        copy.start()
        pending.append(copy)

    def arrived(dst, ssem, rsem):
        pltpu.make_async_remote_copy(
            src_ref=dst, dst_ref=dst, send_sem=ssem, recv_sem=rsem,
            device_id=pair, device_id_type=MESH,
        ).wait_recv()

    def stream_of(layer, c):
        if layer == 0:
            return tokens[c * t:(c + 1) * t, :].astype(jnp.float32)
        return strm[layer - 1, c].astype(jnp.float32).reshape(t, d)

    def ua(layer, c):
        i = layer * chunks + c
        current = stream_of(layer, c)
        squares = current * current
        folded = squares[:, 0:128]
        for j in range(1, d // 128):
            folded = folded + squares[:, j * 128:(j + 1) * 128]
        row = jnp.sum(folded.T, axis=0, keepdims=True)
        sums_out[i] = jnp.broadcast_to(row, (8, t))
        for o in range(1, nr):
            send(sums_out.at[i], sums_in.at[i, o - 1], sums_ss.at[i, o - 1], sums_rs.at[i, o - 1],
                 (ra_peer(o), cb))
        scaled = (current * gain[layer:layer + 1, :]).astype(jnp.bfloat16)
        for g, w in ((0, wg), (1, wv)):
            if c == 0:
                weights[layer][g].wait()
                buf[g, 0:8, :] = jnp.zeros((8, ff), jnp.float32)
            else:
                buf[g, 0:8, :] = buf[g, t:t + 8, :]
            for start, size in lane_tiles(ff):
                buf[g, 8:8 + t, start:start + size] = jnp.dot(
                    scaled, w[layer, :, start:start + size], preferred_element_type=jnp.float32)

    def ub(layer, c):
        i = layer * chunks + c
        total = sums_out[i]
        for o in range(1, nr):
            arrived(sums_in.at[i, o - 1], sums_ss.at[i, o - 1], sums_rs.at[i, o - 1])
            total = total + sums_in[i, o - 1]
        inverse = lax.rsqrt(total / total_d + epsilon)
        inverse = jnp.broadcast_to(inverse[0:1, :], (128, t)).T[:, 0:1]
        for g, taps in ((0, gate_taps), (1, value_taps)):
            for start, size in lane_tiles(ff, 128):
                cols = slice(start, start + size)
                buf[g, 8:8 + t, cols] = buf[g, 8:8 + t, cols] * inverse
                width = taps.shape[1]
                result = None
                for offset in range(width):
                    first = 8 - (width - 1) + offset
                    term = taps[layer, offset:offset + 1, cols] * buf[g, first:first + t, cols]
                    result = term if result is None else result + term
                part[i, g, :, :, cols] = result.reshape(nr, tr, size).astype(jnp.bfloat16)
            for o in range(1, nr):
                send(part.at[i, g, ra_peer(o)], part_in.at[i, g, o - 1],
                     part_ss.at[i, g, o - 1], part_rs.at[i, g, o - 1], (ra_peer(o), cb))

    def h(layer, c):
        i = layer * chunks + c
        for g in range(2):
            for o in range(1, nr):
                arrived(part_in.at[i, g, o - 1], part_ss.at[i, g, o - 1], part_rs.at[i, g, o - 1])
        pair_of = []
        for g in range(2):
            total = part[i, g, r].astype(jnp.float32)
            for o in range(1, nr):
                total = total + part_in[i, g, o - 1].astype(jnp.float32)
            pair_of.append(total)
        gate, value = pair_of
        hid[i, r] = (jax.nn.silu(gate) * value).astype(jnp.bfloat16)
        for o in range(1, nr):
            send(hid.at[i, r], hid.at[i, r], hid_ss.at[i, o - 1], hid_rs.at[i, o - 1],
                 (ra_peer(o), cb))

    def wa(layer, c):
        i = layer * chunks + c
        for o in range(1, nr):
            arrived(hid.at[i, ra_peer(nr - o)], hid_ss.at[i, o - 1], hid_rs.at[i, o - 1])
        if c == 0:
            weights[layer][2].wait()
        hidden = hid[i].reshape(t, ff)
        for start, size in lane_tiles(d):
            branch = jnp.dot(hidden, wd[layer, :, start:start + size],
                             preferred_element_type=jnp.float32)
            acc[c, :, :, start:start + size] = branch.reshape(CORES, t // CORES, size)
        half[i] = acc[c, 1 - k].astype(jnp.bfloat16)
        send(half.at[i], half_in.at[i], half_ss.at[i], half_rs.at[i], pair)

    def wb(layer, c):
        i = layer * chunks + c
        arrived(half_in.at[i], half_ss.at[i], half_rs.at[i])
        total = acc[c, k] + half_in[i].astype(jnp.float32)
        acc[c, k] = total
        red[i] = total.reshape(nz, tz, d).astype(jnp.bfloat16)
        for o in range(1, nz):
            send(red.at[i, z_peer(o)], red_in.at[i, o - 1], red_ss.at[i, o - 1], red_rs.at[i, o - 1],
                 (r, z_peer(o) * CORES + k))

    def sa(layer, c):
        i = layer * chunks + c
        if layer == 0:
            first = c * t + (k * nz + z) * tz
            current = tokens[pl.ds(pl.multiple_of(first, tz), tz), :].astype(jnp.float32)
        else:
            current = strm[layer - 1, c, k, z].astype(jnp.float32)
        total = red[i, z].astype(jnp.float32)
        for o in range(1, nz):
            arrived(red_in.at[i, o - 1], red_ss.at[i, o - 1], red_rs.at[i, o - 1])
            total = total + red_in[i, o - 1].astype(jnp.float32)
        strm[layer, c, k, z] = (0.5 * current + total).astype(jnp.bfloat16)
        for o in range(1, nz):
            mine = strm.at[layer, c, k, z]
            send(mine, mine, strm_ss.at[i, o - 1], strm_rs.at[i, o - 1],
                 (r, z_peer(o) * CORES + k))

    def sb(layer, c):
        i = layer * chunks + c
        for o in range(1, nz):
            arrived(strm.at[layer, c, k, z_peer(nz - o)], strm_ss.at[i, o - 1], strm_rs.at[i, o - 1])
        mine = strm.at[layer, c, k]
        send(mine, mine, pair_ss.at[i], pair_rs.at[i], pair)

    def sc(layer, c):
        i = layer * chunks + c
        arrived(strm.at[layer, c, 1 - k], pair_ss.at[i], pair_rs.at[i])
        if layer == layers - 1:
            final = strm[layer, c].astype(jnp.float32).reshape(t, d)
            out[c * t:(c + 1) * t, :] = final.astype(jnp.bfloat16)

    steps = dict(ua=ua, ub=ub, h=h, wa=wa, wb=wb, sa=sa, sb=sb, sc=sc)
    for name, layer, c in schedule(layers, chunks):
        steps[name](layer, c)
    for copy in pending:
        copy.wait_send()


def body(nr, nc, tokens, norm_gain, gate_weight, value_weight, gate_taps, value_taps, down_weight):
    layers, d, ff = gate_weight.shape
    rows = tokens.shape[0]
    nz = nc // CORES
    chunks = 2 if rows // 2 >= 16 * max(nr, nc) else 1
    t = rows // chunks
    n = layers * chunks
    cfg = (layers, chunks, nr, nz, t, ff, d, d * nr)
    bf16, f32 = jnp.bfloat16, jnp.float32
    dma = pltpu.SemaphoreType.DMA
    vmem = pl.BlockSpec(memory_space=pltpu.VMEM)
    hbm = pl.BlockSpec(memory_space=pltpu.HBM)
    tz = t // nc
    return pl.pallas_call(
        functools.partial(kernel, cfg),
        out_shape=jax.ShapeDtypeStruct((rows, d), bf16),
        in_specs=[vmem, vmem, hbm, hbm, vmem, vmem, hbm],
        out_specs=vmem,
        scratch_shapes=[
            pltpu.VMEM((layers, d, ff), bf16),
            pltpu.VMEM((layers, d, ff), bf16),
            pltpu.VMEM((layers, ff, d), bf16),
            pltpu.VMEM((2, 8 + t, ff), f32),
            pltpu.VMEM((n, 8, t), f32),
            pltpu.VMEM((n, nr - 1, 8, t), f32),
            pltpu.VMEM((n, 2, nr, t // nr, ff), bf16),
            pltpu.VMEM((n, 2, nr - 1, t // nr, ff), bf16),
            pltpu.VMEM((n, nr, t // nr, ff), bf16),
            pltpu.VMEM((chunks, CORES, t // CORES, d), f32),
            pltpu.VMEM((n, t // CORES, d), bf16),
            pltpu.VMEM((n, t // CORES, d), bf16),
            pltpu.VMEM((n, nz, tz, d), bf16),
            pltpu.VMEM((n, nz - 1, tz, d), bf16),
            pltpu.VMEM((layers, chunks, CORES, nz, tz, d), bf16),
            dma((layers, 3)),
            dma((n, nr - 1)), dma((n, nr - 1)),
            dma((n, 2, nr - 1)), dma((n, 2, nr - 1)),
            dma((n, nr - 1)), dma((n, nr - 1)),
            dma((n,)), dma((n,)),
            dma((n, nz - 1)), dma((n, nz - 1)),
            dma((n, nz - 1)), dma((n, nz - 1)),
            dma((n,)), dma((n,)),
        ],
        compiler_params=pltpu.CompilerParams(
            collective_id=0, has_side_effects=True, vmem_limit_bytes=60 * 1024 * 1024,
        ),
    )(tokens, norm_gain, gate_weight, value_weight, gate_taps, value_taps, down_weight)


def solution(mesh):
    return jax.shard_map(
        functools.partial(body, mesh.shape["ra"], mesh.shape["cb"]),
        mesh=mesh,
        in_specs=(
            P(None, "ra"),
            P(None, "ra"),
            P(None, "ra", "cb"),
            P(None, "ra", "cb"),
            P(None, None, "cb"),
            P(None, None, "cb"),
            P(None, "cb", "ra"),
        ),
        out_specs=P(None, "ra"),
        check_vma=False,
    )
```

```python
import functools

import jax
import jax.numpy as jnp
from jax import lax
from jax.experimental import pallas as pl
from jax.experimental.pallas import tpu as pltpu
from jax.sharding import PartitionSpec as P

epsilon = 1e-06
MESH = pl.DeviceIdType.MESH
CORES = 2


def lane_tiles(width, tile=512):
    return [(start, min(tile, width - start)) for start in range(0, width, tile)]


STAGES = dict(u=0.0, x2=7.0, h=10.5, g2=14.0, wa=17.0, wb=19.5, sa=24.0, sb=28.5, sc=30.0)
LAYER_TIME = 32.0
CHUNK_TIME = 4.0


def schedule(layers, chunks):
    steps = [
        (layer * LAYER_TIME + c * CHUNK_TIME + when, layer, c, name)
        for layer in range(layers) for c in range(chunks) for name, when in STAGES.items()
    ]
    return [(name, layer, c) for _, layer, c, name in sorted(steps)]


def kernel(
    cfg,
    tokens, gain, gate_hbm, value_hbm, gate_taps, value_taps, down_hbm,
    out,
    wg, wv, wd, buf, sums_out, sums_in, part, gate_one, value_one, mid, gate_two, value_two,
    hid, acc, half, half_in, red, red_in, strm,
    w_sem, sums_ss, sums_rs, g1_ss, g1_rs, v1_ss, v1_rs, g2_ss, g2_rs, v2_ss, v2_rs,
    ax1_ss, ax1_rs, ay1_ss, ay1_rs, ax2_ss, ax2_rs, ay2_ss, ay2_rs,
    half_ss, half_rs, red_ss, red_rs, strm_ss, strm_rs, pair_ss, pair_rs,
):
    layers, chunks, ny, nx, nz, t, ff, d, total_d = cfg
    nr = ny * nx
    tr = t // nr
    tz = t // (CORES * nz)
    r = lax.axis_index("ra")
    cb = lax.axis_index("cb")
    z, k = cb // CORES, lax.rem(cb, CORES)
    pair = (r, z * CORES + 1 - k)
    y, x = r // nx, lax.rem(r, nx)

    def y_peer(off):
        return lax.rem(y + off, ny)

    def x_peer(off):
        return lax.rem(x + off, nx)

    def at_y(row):
        return (row * nx + x, cb)

    def at_x(column):
        return (y * nx + column, cb)

    def ra_peer(off):
        return lax.rem(r + off, nr)

    def z_peer(off):
        return lax.rem(z + off, nz)

    def weight_copies(layer):
        return [
            pltpu.make_async_copy(src.at[layer], dst.at[layer], w_sem.at[layer, i])
            for i, (src, dst) in enumerate(((gate_hbm, wg), (value_hbm, wv), (down_hbm, wd)))
        ]

    weights = [weight_copies(layer) for layer in range(layers)]
    for copies in weights:
        for copy in copies:
            copy.start()

    barrier = pltpu.get_barrier_semaphore()
    peers = [(ra_peer(o), cb) for o in range(1, nr)]
    peers += [(r, z_peer(o) * CORES + k) for o in range(1, nz)] + [pair]
    for peer in peers:
        pl.semaphore_signal(barrier, inc=1, device_id=peer, device_id_type=MESH)
    pl.semaphore_wait(barrier, len(peers))

    pending = []

    def send(src, dst, ssem, rsem, device):
        copy = pltpu.make_async_remote_copy(
            src_ref=src, dst_ref=dst, send_sem=ssem, recv_sem=rsem,
            device_id=device, device_id_type=MESH,
        )
        copy.start()
        pending.append(copy)

    def arrived(dst, ssem, rsem):
        pltpu.make_async_remote_copy(
            src_ref=dst, dst_ref=dst, send_sem=ssem, recv_sem=rsem,
            device_id=pair, device_id_type=MESH,
        ).wait_recv()

    def stream_of(layer, c):
        if layer == 0:
            return tokens[c * t:(c + 1) * t, :].astype(jnp.float32)
        return strm[layer - 1, c].astype(jnp.float32).reshape(t, d)

    def u(layer, c):
        ua(layer, c)
        ub(layer, c)

    def ua(layer, c):
        i = layer * chunks + c
        current = stream_of(layer, c)
        squares = current * current
        folded = squares[:, 0:128]
        for j in range(1, d // 128):
            folded = folded + squares[:, j * 128:(j + 1) * 128]
        row = jnp.sum(folded.T, axis=0, keepdims=True)
        sums_out[i] = jnp.broadcast_to(row, (8, t))
        for o in range(1, nr):
            send(sums_out.at[i], sums_in.at[i, o - 1], sums_ss.at[i, o - 1], sums_rs.at[i, o - 1],
                 (ra_peer(o), cb))
        scaled = (current * gain[layer:layer + 1, :]).astype(jnp.bfloat16)
        for g, w in ((0, wg), (1, wv)):
            if c == 0:
                weights[layer][g].wait()
                buf[layer, g, 0:8, :] = jnp.zeros((8, ff), jnp.float32)
            else:
                buf[layer, g, 0:8, :] = buf[layer, g, t:t + 8, :]
            for start, size in lane_tiles(ff):
                buf[layer, g, 8:8 + t, start:start + size] = lax.dot_general(
                    scaled, w[layer, start:start + size, :], (((1,), (1,)), ((), ())),
                    preferred_element_type=jnp.float32)

    def ub(layer, c):
        i = layer * chunks + c
        total = sums_out[i]
        for o in range(1, nr):
            arrived(sums_in.at[i, o - 1], sums_ss.at[i, o - 1], sums_rs.at[i, o - 1])
            total = total + sums_in[i, o - 1]
        inverse = lax.rsqrt(total / total_d + epsilon)
        inverse = jnp.broadcast_to(inverse[0:1, :], (128, t)).T[:, 0:1]
        for g, taps in ((0, gate_taps), (1, value_taps)):
            for start, size in lane_tiles(ff, 128):
                cols = slice(start, start + size)
                buf[layer, g, 8:8 + t, cols] = buf[layer, g, 8:8 + t, cols] * inverse
                width = taps.shape[0]
                result = None
                for offset in range(width):
                    first = 8 - (width - 1) + offset
                    term = taps[offset, layer:layer + 1, cols] * buf[layer, g, first:first + t, cols]
                    result = term if result is None else result + term
                part[i, g, :, :, :, cols] = result.reshape(ny, nx, tr, size).astype(jnp.bfloat16)
            if g == 0:
                for o in range(1, nx):
                    send(part.at[i, 0, :, x_peer(o)], gate_one.at[i, o - 1],
                         g1_ss.at[i, o - 1], g1_rs.at[i, o - 1], at_x(x_peer(o)))
            else:
                for o in range(1, ny):
                    send(part.at[i, 1, y_peer(o)], value_one.at[i, o - 1],
                         v1_ss.at[i, o - 1], v1_rs.at[i, o - 1], at_y(y_peer(o)))

    def gate_sum(i, row):
        total = part[i, 0, row, x].astype(jnp.float32)
        for o in range(1, nx):
            total = total + gate_one[i, o - 1, row].astype(jnp.float32)
        return total

    def value_sum(i, column):
        total = part[i, 1, y, column].astype(jnp.float32)
        for o in range(1, ny):
            total = total + value_one[i, o - 1, column].astype(jnp.float32)
        return total

    def x2(layer, c):
        i = layer * chunks + c
        for o in range(1, nx):
            arrived(gate_one.at[i, o - 1], g1_ss.at[i, o - 1], g1_rs.at[i, o - 1])
        for o in range(1, ny):
            mid[i, 0, o - 1] = gate_sum(i, y_peer(o)).astype(jnp.bfloat16)
            send(mid.at[i, 0, o - 1], gate_two.at[i, o - 1],
                 g2_ss.at[i, o - 1], g2_rs.at[i, o - 1], at_y(y_peer(o)))
        for o in range(1, ny):
            arrived(value_one.at[i, o - 1], v1_ss.at[i, o - 1], v1_rs.at[i, o - 1])
        for o in range(1, nx):
            mid[i, 1, o - 1] = value_sum(i, x_peer(o)).astype(jnp.bfloat16)
            send(mid.at[i, 1, o - 1], value_two.at[i, o - 1],
                 v2_ss.at[i, o - 1], v2_rs.at[i, o - 1], at_x(x_peer(o)))

    def h(layer, c):
        i = layer * chunks + c
        gate = gate_sum(i, y)
        for o in range(1, ny):
            arrived(gate_two.at[i, o - 1], g2_ss.at[i, o - 1], g2_rs.at[i, o - 1])
            gate = gate + gate_two[i, o - 1].astype(jnp.float32)
        value = value_sum(i, x)
        for o in range(1, nx):
            arrived(value_two.at[i, o - 1], v2_ss.at[i, o - 1], v2_rs.at[i, o - 1])
            value = value + value_two[i, o - 1].astype(jnp.float32)
        hidden = (jax.nn.silu(gate) * value).reshape(2, tr // 2, ff)
        hid[i, y, x] = hidden.astype(jnp.bfloat16)
        for o in range(1, nx):
            mine = hid.at[i, y, x, 0]
            send(mine, mine, ax1_ss.at[i, o - 1], ax1_rs.at[i, o - 1], at_x(x_peer(o)))
        for o in range(1, ny):
            mine = hid.at[i, y, x, 1]
            send(mine, mine, ay1_ss.at[i, o - 1], ay1_rs.at[i, o - 1], at_y(y_peer(o)))

    def g2(layer, c):
        i = layer * chunks + c
        for o in range(1, nx):
            arrived(hid.at[i, y, x_peer(nx - o), 0], ax1_ss.at[i, o - 1], ax1_rs.at[i, o - 1])
        for o in range(1, ny):
            mine = hid.at[i, y, :, 0]
            send(mine, mine, ay2_ss.at[i, o - 1], ay2_rs.at[i, o - 1], at_y(y_peer(o)))
        for o in range(1, ny):
            arrived(hid.at[i, y_peer(ny - o), x, 1], ay1_ss.at[i, o - 1], ay1_rs.at[i, o - 1])
        for o in range(1, nx):
            mine = hid.at[i, :, x, 1]
            send(mine, mine, ax2_ss.at[i, o - 1], ax2_rs.at[i, o - 1], at_x(x_peer(o)))

    def wa(layer, c):
        i = layer * chunks + c
        for o in range(1, ny):
            arrived(hid.at[i, y_peer(ny - o), :, 0], ay2_ss.at[i, o - 1], ay2_rs.at[i, o - 1])
        for o in range(1, nx):
            arrived(hid.at[i, :, x_peer(nx - o), 1], ax2_ss.at[i, o - 1], ax2_rs.at[i, o - 1])
        if c == 0:
            weights[layer][2].wait()
        hidden = hid[i].reshape(t, ff)
        for start, size in lane_tiles(d):
            branch = jnp.dot(hidden, wd[layer, :, start:start + size],
                             preferred_element_type=jnp.float32)
            acc[c, :, :, start:start + size] = branch.reshape(CORES, t // CORES, size)
        half[i] = acc[c, 1 - k].astype(jnp.bfloat16)
        send(half.at[i], half_in.at[i], half_ss.at[i], half_rs.at[i], pair)

    def wb(layer, c):
        i = layer * chunks + c
        arrived(half_in.at[i], half_ss.at[i], half_rs.at[i])
        total = acc[c, k] + half_in[i].astype(jnp.float32)
        acc[c, k] = total
        red[i] = total.reshape(nz, tz, d).astype(jnp.bfloat16)
        for o in range(1, nz):
            send(red.at[i, z_peer(o)], red_in.at[i, o - 1], red_ss.at[i, o - 1], red_rs.at[i, o - 1],
                 (r, z_peer(o) * CORES + k))

    def sa(layer, c):
        i = layer * chunks + c
        if layer == 0:
            first = c * t + (k * nz + z) * tz
            current = tokens[pl.ds(pl.multiple_of(first, tz), tz), :].astype(jnp.float32)
        else:
            current = strm[layer - 1, c, k, z].astype(jnp.float32)
        total = red[i, z].astype(jnp.float32)
        for o in range(1, nz):
            arrived(red_in.at[i, o - 1], red_ss.at[i, o - 1], red_rs.at[i, o - 1])
            total = total + red_in[i, o - 1].astype(jnp.float32)
        strm[layer, c, k, z] = (0.5 * current + total).astype(jnp.bfloat16)
        for o in range(1, nz):
            mine = strm.at[layer, c, k, z]
            send(mine, mine, strm_ss.at[i, o - 1], strm_rs.at[i, o - 1],
                 (r, z_peer(o) * CORES + k))

    def sb(layer, c):
        i = layer * chunks + c
        for o in range(1, nz):
            arrived(strm.at[layer, c, k, z_peer(nz - o)], strm_ss.at[i, o - 1], strm_rs.at[i, o - 1])
        mine = strm.at[layer, c, k]
        send(mine, mine, pair_ss.at[i], pair_rs.at[i], pair)

    def sc(layer, c):
        i = layer * chunks + c
        arrived(strm.at[layer, c, 1 - k], pair_ss.at[i], pair_rs.at[i])
        if layer == layers - 1:
            final = strm[layer, c].astype(jnp.float32).reshape(t, d)
            out[c * t:(c + 1) * t, :] = final.astype(jnp.bfloat16)

    steps = dict(u=u, x2=x2, h=h, g2=g2, wa=wa, wb=wb, sa=sa, sb=sb, sc=sc)
    for name, layer, c in schedule(layers, chunks):
        steps[name](layer, c)
    for copy in pending:
        copy.wait_send()


def body(nr, nc, tokens, norm_gain, gate_weight, value_weight, gate_taps, value_taps, down_weight):
    layers, d, ff = gate_weight.shape
    gate_weight, value_weight = (jnp.swapaxes(w, 1, 2) for w in (gate_weight, value_weight))
    gate_taps, value_taps = (jnp.swapaxes(w, 0, 1) for w in (gate_taps, value_taps))
    ny = max(f for f in range(1, nr + 1) if nr % f == 0 and f * f <= nr)
    nx = nr // ny
    rows = tokens.shape[0]
    nz = nc // CORES
    chunks = 2 if rows // 2 >= 16 * max(nr, nc) else 1
    t = rows // chunks
    n = layers * chunks
    cfg = (layers, chunks, ny, nx, nz, t, ff, d, d * nr)
    bf16, f32 = jnp.bfloat16, jnp.float32
    dma = pltpu.SemaphoreType.DMA
    vmem = pl.BlockSpec(memory_space=pltpu.VMEM)
    hbm = pl.BlockSpec(memory_space=pltpu.HBM)
    tz, tr = t // nc, t // nr
    px, py = max(nx - 1, 1), max(ny - 1, 1)
    return pl.pallas_call(
        functools.partial(kernel, cfg),
        out_shape=jax.ShapeDtypeStruct((rows, d), bf16),
        in_specs=[vmem, vmem, hbm, hbm, vmem, vmem, hbm],
        out_specs=vmem,
        scratch_shapes=[
            pltpu.VMEM((layers, ff, d), bf16),
            pltpu.VMEM((layers, ff, d), bf16),
            pltpu.VMEM((layers, ff, d), bf16),
            pltpu.VMEM((layers, 2, 8 + t, ff), f32),
            pltpu.VMEM((n, 8, t), f32),
            pltpu.VMEM((n, nr - 1, 8, t), f32),
            pltpu.VMEM((n, 2, ny, nx, tr, ff), bf16),
            pltpu.VMEM((n, px, ny, tr, ff), bf16),
            pltpu.VMEM((n, py, nx, tr, ff), bf16),
            pltpu.VMEM((n, 2, max(px, py), tr, ff), bf16),
            pltpu.VMEM((n, py, tr, ff), bf16),
            pltpu.VMEM((n, px, tr, ff), bf16),
            pltpu.VMEM((n, ny, nx, 2, tr // 2, ff), bf16),
            pltpu.VMEM((chunks, CORES, t // CORES, d), f32),
            pltpu.VMEM((n, t // CORES, d), bf16),
            pltpu.VMEM((n, t // CORES, d), bf16),
            pltpu.VMEM((n, nz, tz, d), bf16),
            pltpu.VMEM((n, nz - 1, tz, d), bf16),
            pltpu.VMEM((layers, chunks, CORES, nz, tz, d), bf16),
            dma((layers, 3)),
            dma((n, nr - 1)), dma((n, nr - 1)),
            dma((n, px)), dma((n, px)), dma((n, py)), dma((n, py)),
            dma((n, py)), dma((n, py)), dma((n, px)), dma((n, px)),
            dma((n, px)), dma((n, px)), dma((n, py)), dma((n, py)),
            dma((n, px)), dma((n, px)), dma((n, py)), dma((n, py)),
            dma((n,)), dma((n,)),
            dma((n, nz - 1)), dma((n, nz - 1)),
            dma((n, nz - 1)), dma((n, nz - 1)),
            dma((n,)), dma((n,)),
        ],
        compiler_params=pltpu.CompilerParams(
            collective_id=0, has_side_effects=True, vmem_limit_bytes=60 * 1024 * 1024,
        ),
    )(tokens, norm_gain, gate_weight, value_weight, gate_taps, value_taps, down_weight)


def solution(mesh):
    return jax.shard_map(
        functools.partial(body, mesh.shape["ra"], mesh.shape["cb"]),
        mesh=mesh,
        in_specs=(
            P(None, "ra"),
            P(None, "ra"),
            P(None, "ra", "cb"),
            P(None, "ra", "cb"),
            P(None, None, "cb"),
            P(None, None, "cb"),
            P(None, "cb", "ra"),
        ),
        out_specs=P(None, "ra"),
        check_vma=False,
    )
```

```python
import functools

import jax
import jax.numpy as jnp
from jax import lax
from jax.experimental import pallas as pl
from jax.experimental.pallas import tpu as pltpu
from jax.sharding import PartitionSpec as P

epsilon = 1e-06
MESH = pl.DeviceIdType.MESH
CORES = 2
LANES = 128


def lane_tiles(width, tile=512):
    return [(start, min(tile, width - start)) for start in range(0, width, tile)]


LINK_RATE = 46000.0
PAIR_RATE = 300000.0
LATENCY = 2.0
STAGGER = 0.0
PAIR_LATENCY = 1.1
WORK = dict(s=0.2, u=2.0, x2=0.5, h=0.5, g2=0.1, wa=0.7, wb=0.2, sa=0.2, sb=0.1, sc=0.1)


def schedule(layers, chunks, ny, nx, nz, t, ff, d):
    nr = ny * nx
    third = max(1.0, (nz * nz) / 4.0)
    up = 2.0 * t * ff / nr
    down = 2.0 * t * d / (CORES * nz)
    sends = dict(
        s=dict(x=100.0, y=100.0),
        u=dict(x=up * ny * (nx - 1), y=up * nx * (ny - 1)),
        x2=dict(y=up * (ny - 1), x=up * (nx - 1)),
        h=dict(x=up / 2 * (nx - 1), y=up / 2 * (ny - 1)),
        g2=dict(x=up / 2 * ny * (nx - 1), y=up / 2 * nx * (ny - 1)),
        wa=dict(p=down * nz),
        wb=dict(z=down * third),
        sa=dict(z=down * third),
        sb=dict(p=down * nz),
        sc=dict(),
    )
    names = list(sends)
    free = dict(x=0.0, y=0.0, z=0.0, p=0.0)
    ready = {c: c * STAGGER for c in range(chunks)}
    place = {c: 0 for c in range(chunks)}
    now, order, depth = 0.0, [], len(names)
    while len(order) < layers * chunks * depth:
        open_chunks = []
        for c in range(chunks):
            if place[c] == layers * depth:
                continue
            if names[place[c] % depth] == "u" and c and place[c - 1] <= place[c]:
                continue
            open_chunks.append((max(ready[c], now), c))
        when, c = min(open_chunks)
        name = names[place[c] % depth]
        order.append((name, place[c] // depth, c))
        place[c] += 1
        now = when + WORK[name] * t / 128
        ready[c] = now
        for link, size in sends[name].items():
            rate, lag = (PAIR_RATE, PAIR_LATENCY) if link == "p" else (LINK_RATE, LATENCY)
            free[link] = max(free[link], now) + size / rate
            ready[c] = max(ready[c], free[link] + lag)
    return order


def kernel(
    cfg,
    tokens, gain, gate_hbm, value_hbm, gate_taps, value_taps, down_hbm,
    out,
    wg, wv, wd, turned, buf, sums_out, sums_in, part, gate_one, value_one, mid, gate_two, value_two,
    hid, acc, half, half_in, red, red_in, strm,
    w_sem, sums_ss, sums_rs, g1_ss, g1_rs, v1_ss, v1_rs, g2_ss, g2_rs, v2_ss, v2_rs,
    ax1_ss, ax1_rs, ay1_ss, ay1_rs, ax2_ss, ax2_rs, ay2_ss, ay2_rs,
    half_ss, half_rs, red_ss, red_rs, strm_ss, strm_rs, pair_ss, pair_rs,
):
    layers, chunks, ny, nx, nz, t, ff, d, total_d = cfg
    nr = ny * nx
    tr = t // nr
    tz = t // (CORES * nz)
    r = lax.axis_index("ra")
    cb = lax.axis_index("cb")
    z, k = cb // CORES, lax.rem(cb, CORES)
    pair = (r, z * CORES + 1 - k)
    y, x = r // nx, lax.rem(r, nx)

    def y_peer(off):
        return lax.rem(y + off, ny)

    def x_peer(off):
        return lax.rem(x + off, nx)

    def at_y(row):
        return (row * nx + x, cb)

    def at_x(column):
        return (y * nx + column, cb)

    def ra_peer(off):
        return lax.rem(r + off, nr)

    def z_peer(off):
        return lax.rem(z + off, nz)

    def weight_copies(layer):
        return [
            pltpu.make_async_copy(src.at[layer], dst.at[layer], w_sem.at[layer, i])
            for i, (src, dst) in enumerate(((gate_hbm, wg), (value_hbm, wv), (down_hbm, wd)))
        ]

    weights = [weight_copies(layer) for layer in range(layers)]
    for copy in weights[0][:2]:
        copy.start()

    barrier = pltpu.get_barrier_semaphore()
    peers = [(ra_peer(o), cb) for o in range(1, nr)]
    peers += [(r, z_peer(o) * CORES + k) for o in range(1, nz)] + [pair]
    for peer in peers:
        pl.semaphore_signal(barrier, inc=1, device_id=peer, device_id_type=MESH)
    pl.semaphore_wait(barrier, len(peers))

    pending = []

    def send(src, dst, ssem, rsem, device):
        copy = pltpu.make_async_remote_copy(
            src_ref=src, dst_ref=dst, send_sem=ssem, recv_sem=rsem,
            device_id=device, device_id_type=MESH,
        )
        copy.start()
        pending.append(copy)

    def arrived(dst, ssem, rsem):
        pltpu.make_async_remote_copy(
            src_ref=dst, dst_ref=dst, send_sem=ssem, recv_sem=rsem,
            device_id=pair, device_id_type=MESH,
        ).wait_recv()

    def stream_of(layer, c):
        if layer == 0:
            return tokens[c * t:(c + 1) * t, :].astype(jnp.float32)
        return strm[layer - 1, c].astype(jnp.float32).reshape(t, d)

    def s(layer, c):
        i = layer * chunks + c
        current = stream_of(layer, c)
        squares = current * current
        folded = squares[:, 0:128]
        for j in range(1, d // 128):
            folded = folded + squares[:, j * 128:(j + 1) * 128]
        row = jnp.sum(folded.T, axis=0, keepdims=True)
        sums_out[i] = jnp.broadcast_to(row, (8, t))
        for o in range(1, nr):
            send(sums_out.at[i], sums_in.at[i, o - 1], sums_ss.at[i, o - 1], sums_rs.at[i, o - 1],
                 (ra_peer(o), cb))

    def turn(layer):
        for g, w in ((0, wg), (1, wv)):
            weights[layer][g].wait()
            for start, size in lane_tiles(ff, 128):
                turned[layer - 1, g, :, start:start + size] = w[layer, start:start + size, :].T

    def u(layer, c):
        i = layer * chunks + c
        current = stream_of(layer, c)
        scaled = (current * gain[layer:layer + 1, :]).astype(jnp.bfloat16)
        for g, w in ((0, wg), (1, wv)):
            if c == 0:
                if layer == 0:
                    weights[layer][g].wait()
                    later = [weights[0][2]] if g == 0 else [w for ws in weights[1:] for w in ws]
                    for copy in later:
                        copy.start()
                buf[layer, g, 0:8, :] = jnp.zeros((8, ff), jnp.float32)
            else:
                buf[layer, g, 0:8, :] = buf[layer, g, t:t + 8, :]
            for start, size in lane_tiles(ff):
                if layer:
                    product = jnp.dot(scaled, turned[layer - 1, g, :, start:start + size],
                                      preferred_element_type=jnp.float32)
                else:
                    product = lax.dot_general(
                        scaled, w[layer, start:start + size, :], (((1,), (1,)), ((), ())),
                        preferred_element_type=jnp.float32)
                buf[layer, g, 8:8 + t, start:start + size] = product

        total = sums_out[i]
        for o in range(1, nr):
            arrived(sums_in.at[i, o - 1], sums_ss.at[i, o - 1], sums_rs.at[i, o - 1])
            total = total + sums_in[i, o - 1]
        inverse = lax.rsqrt(total / total_d + epsilon)
        inverse = jnp.broadcast_to(inverse[0:1, :], (128, t)).T[:, 0:1]
        for g, taps in ((0, gate_taps), (1, value_taps)):
            for start, size in lane_tiles(ff, 128):
                cols = slice(start, start + size)
                buf[layer, g, 8:8 + t, cols] = buf[layer, g, 8:8 + t, cols] * inverse
                width = taps.shape[0]
                result = None
                for offset in range(width):
                    first = 8 - (width - 1) + offset
                    term = taps[offset, layer:layer + 1, cols] * buf[layer, g, first:first + t, cols]
                    result = term if result is None else result + term
                part[i, g, :, :, :, cols] = result.reshape(ny, nx, tr, size).astype(jnp.bfloat16)
            if g == 0:
                for o in range(1, nx):
                    send(part.at[i, 0, :, x_peer(o)], gate_one.at[i, o - 1],
                         g1_ss.at[i, o - 1], g1_rs.at[i, o - 1], at_x(x_peer(o)))
            else:
                for o in range(1, ny):
                    send(part.at[i, 1, y_peer(o)], value_one.at[i, o - 1],
                         v1_ss.at[i, o - 1], v1_rs.at[i, o - 1], at_y(y_peer(o)))

    def gate_sum(i, row):
        total = part[i, 0, row, x].astype(jnp.float32)
        for o in range(1, nx):
            total = total + gate_one[i, o - 1, row].astype(jnp.float32)
        return total

    def value_sum(i, column):
        total = part[i, 1, y, column].astype(jnp.float32)
        for o in range(1, ny):
            total = total + value_one[i, o - 1, column].astype(jnp.float32)
        return total

    def x2(layer, c):
        i = layer * chunks + c
        for o in range(1, nx):
            arrived(gate_one.at[i, o - 1], g1_ss.at[i, o - 1], g1_rs.at[i, o - 1])
        for o in range(1, ny):
            mid[i, 0, o - 1] = gate_sum(i, y_peer(o)).astype(jnp.bfloat16)
            send(mid.at[i, 0, o - 1], gate_two.at[i, o - 1],
                 g2_ss.at[i, o - 1], g2_rs.at[i, o - 1], at_y(y_peer(o)))
        for o in range(1, ny):
            arrived(value_one.at[i, o - 1], v1_ss.at[i, o - 1], v1_rs.at[i, o - 1])
        for o in range(1, nx):
            mid[i, 1, o - 1] = value_sum(i, x_peer(o)).astype(jnp.bfloat16)
            send(mid.at[i, 1, o - 1], value_two.at[i, o - 1],
                 v2_ss.at[i, o - 1], v2_rs.at[i, o - 1], at_x(x_peer(o)))

    def h(layer, c):
        i = layer * chunks + c
        gate = gate_sum(i, y)
        for o in range(1, ny):
            arrived(gate_two.at[i, o - 1], g2_ss.at[i, o - 1], g2_rs.at[i, o - 1])
            gate = gate + gate_two[i, o - 1].astype(jnp.float32)
        value = value_sum(i, x)
        for o in range(1, nx):
            arrived(value_two.at[i, o - 1], v2_ss.at[i, o - 1], v2_rs.at[i, o - 1])
            value = value + value_two[i, o - 1].astype(jnp.float32)
        hidden = (jax.nn.silu(gate) * value).reshape(2, tr // 2, -1)
        hid[i, y, x] = hidden.astype(jnp.bfloat16)
        for o in range(1, nx):
            mine = hid.at[i, y, x, 0]
            send(mine, mine, ax1_ss.at[i, o - 1], ax1_rs.at[i, o - 1], at_x(x_peer(o)))
        for o in range(1, ny):
            mine = hid.at[i, y, x, 1]
            send(mine, mine, ay1_ss.at[i, o - 1], ay1_rs.at[i, o - 1], at_y(y_peer(o)))

    def g2(layer, c):
        i = layer * chunks + c
        for o in range(1, nx):
            arrived(hid.at[i, y, x_peer(nx - o), 0], ax1_ss.at[i, o - 1], ax1_rs.at[i, o - 1])
        for o in range(1, ny):
            mine = hid.at[i, y, :, 0]
            send(mine, mine, ay2_ss.at[i, o - 1], ay2_rs.at[i, o - 1], at_y(y_peer(o)))
        for o in range(1, ny):
            arrived(hid.at[i, y_peer(ny - o), x, 1], ay1_ss.at[i, o - 1], ay1_rs.at[i, o - 1])
        for o in range(1, nx):
            mine = hid.at[i, :, x, 1]
            send(mine, mine, ax2_ss.at[i, o - 1], ax2_rs.at[i, o - 1], at_x(x_peer(o)))

    def wa(layer, c):
        i = layer * chunks + c
        for o in range(1, ny):
            arrived(hid.at[i, y_peer(ny - o), :, 0], ay2_ss.at[i, o - 1], ay2_rs.at[i, o - 1])
        for o in range(1, nx):
            arrived(hid.at[i, :, x_peer(nx - o), 1], ax2_ss.at[i, o - 1], ax2_rs.at[i, o - 1])
        if c == 0:
            weights[layer][2].wait()
        hidden = hid[i].reshape(t, -1)[:, :ff]
        for start, size in lane_tiles(d):
            branch = jnp.dot(hidden, wd[layer, :, start:start + size],
                             preferred_element_type=jnp.float32)
            acc[c, :, :, start:start + size] = branch.reshape(CORES, t // CORES, size)
        half[i] = acc[c, 1 - k].astype(jnp.bfloat16)
        send(half.at[i], half_in.at[i], half_ss.at[i], half_rs.at[i], pair)

    def wb(layer, c):
        i = layer * chunks + c
        arrived(half_in.at[i], half_ss.at[i], half_rs.at[i])
        total = acc[c, k] + half_in[i].astype(jnp.float32)
        acc[c, k] = total
        red[i] = total.reshape(nz, tz, d).astype(jnp.bfloat16)
        for o in range(1, nz):
            send(red.at[i, z_peer(o)], red_in.at[i, o - 1], red_ss.at[i, o - 1], red_rs.at[i, o - 1],
                 (r, z_peer(o) * CORES + k))

    def sa(layer, c):
        i = layer * chunks + c
        if layer == 0:
            first = c * t + (k * nz + z) * tz
            current = tokens[pl.ds(pl.multiple_of(first, tz), tz), :].astype(jnp.float32)
        else:
            current = strm[layer - 1, c, k, z].astype(jnp.float32)
        total = red[i, z].astype(jnp.float32)
        for o in range(1, nz):
            arrived(red_in.at[i, o - 1], red_ss.at[i, o - 1], red_rs.at[i, o - 1])
            total = total + red_in[i, o - 1].astype(jnp.float32)
        strm[layer, c, k, z] = (0.5 * current + total).astype(jnp.bfloat16)
        for o in range(1, nz):
            mine = strm.at[layer, c, k, z]
            send(mine, mine, strm_ss.at[i, o - 1], strm_rs.at[i, o - 1],
                 (r, z_peer(o) * CORES + k))

    def sb(layer, c):
        i = layer * chunks + c
        for o in range(1, nz):
            arrived(strm.at[layer, c, k, z_peer(nz - o)], strm_ss.at[i, o - 1], strm_rs.at[i, o - 1])
        mine = strm.at[layer, c, k]
        send(mine, mine, pair_ss.at[i], pair_rs.at[i], pair)

    def sc(layer, c):
        i = layer * chunks + c
        arrived(strm.at[layer, c, 1 - k], pair_ss.at[i], pair_rs.at[i])
        if layer == layers - 1:
            final = strm[layer, c].astype(jnp.float32).reshape(t, d)
            out[c * t:(c + 1) * t, :] = final.astype(jnp.bfloat16)

    steps = dict(s=s, u=u, x2=x2, h=h, g2=g2, wa=wa, wb=wb, sa=sa, sb=sb, sc=sc)
    for name, layer, c in schedule(layers, chunks, ny, nx, nz, t, ff, d):
        steps[name](layer, c)
        if name == "wb" and c == chunks - 1 and layer + 1 < layers:
            turn(layer + 1)
    for copy in pending:
        copy.wait_send()


def body(nr, nc, tokens, norm_gain, gate_weight, value_weight, gate_taps, value_taps, down_weight):
    layers, d, ff = gate_weight.shape
    gate_weight, value_weight = (jnp.swapaxes(w, 1, 2) for w in (gate_weight, value_weight))
    gate_taps, value_taps = (jnp.swapaxes(w, 0, 1) for w in (gate_taps, value_taps))
    ny = max(f for f in range(1, nr + 1) if nr % f == 0 and f * f <= nr)
    nx = nr // ny
    rows = tokens.shape[0]
    nz = nc // CORES
    chunks = max(c for c in (1, 2, 4) if c == 1 or rows // c >= 8 * max(2 * nr, nc))
    t = rows // chunks
    n = layers * chunks
    cfg = (layers, chunks, ny, nx, nz, t, ff, d, d * nr)
    bf16, f32 = jnp.bfloat16, jnp.float32
    dma = pltpu.SemaphoreType.DMA
    vmem = pl.BlockSpec(memory_space=pltpu.VMEM)
    hbm = pl.BlockSpec(memory_space=pltpu.HBM)
    wide = -(-ff // LANES) * LANES
    tz, tr = t // nc, t // nr
    px, py = max(nx - 1, 1), max(ny - 1, 1)
    return pl.pallas_call(
        functools.partial(kernel, cfg),
        out_shape=jax.ShapeDtypeStruct((rows, d), bf16),
        in_specs=[vmem, vmem, hbm, hbm, vmem, vmem, hbm],
        out_specs=vmem,
        scratch_shapes=[
            pltpu.VMEM((layers, ff, d), bf16),
            pltpu.VMEM((layers, ff, d), bf16),
            pltpu.VMEM((layers, ff, d), bf16),
            pltpu.VMEM((max(layers - 1, 1), 2, d, ff), bf16),
            pltpu.VMEM((layers, 2, 8 + t, ff), f32),
            pltpu.VMEM((n, 8, t), f32),
            pltpu.VMEM((n, nr - 1, 8, t), f32),
            pltpu.VMEM((n, 2, ny, nx, tr, wide), bf16),
            pltpu.VMEM((n, px, ny, tr, wide), bf16),
            pltpu.VMEM((n, py, nx, tr, wide), bf16),
            pltpu.VMEM((n, 2, max(px, py), tr, wide), bf16),
            pltpu.VMEM((n, py, tr, wide), bf16),
            pltpu.VMEM((n, px, tr, wide), bf16),
            pltpu.VMEM((n, ny, nx, 2, tr // 2, wide), bf16),
            pltpu.VMEM((chunks, CORES, t // CORES, d), f32),
            pltpu.VMEM((n, t // CORES, d), bf16),
            pltpu.VMEM((n, t // CORES, d), bf16),
            pltpu.VMEM((n, nz, tz, d), bf16),
            pltpu.VMEM((n, nz - 1, tz, d), bf16),
            pltpu.VMEM((layers, chunks, CORES, nz, tz, d), bf16),
            dma((layers, 3)),
            dma((n, nr - 1)), dma((n, nr - 1)),
            dma((n, px)), dma((n, px)), dma((n, py)), dma((n, py)),
            dma((n, py)), dma((n, py)), dma((n, px)), dma((n, px)),
            dma((n, px)), dma((n, px)), dma((n, py)), dma((n, py)),
            dma((n, px)), dma((n, px)), dma((n, py)), dma((n, py)),
            dma((n,)), dma((n,)),
            dma((n, nz - 1)), dma((n, nz - 1)),
            dma((n, nz - 1)), dma((n, nz - 1)),
            dma((n,)), dma((n,)),
        ],
        compiler_params=pltpu.CompilerParams(
            collective_id=0, has_side_effects=True, vmem_limit_bytes=60 * 1024 * 1024,
        ),
    )(tokens, norm_gain, gate_weight, value_weight, gate_taps, value_taps, down_weight)


def solution(mesh):
    return jax.shard_map(
        functools.partial(body, mesh.shape["ra"], mesh.shape["cb"]),
        mesh=mesh,
        in_specs=(
            P(None, "ra"),
            P(None, "ra"),
            P(None, "ra", "cb"),
            P(None, "ra", "cb"),
            P(None, None, "cb"),
            P(None, None, "cb"),
            P(None, "cb", "ra"),
        ),
        out_specs=P(None, "ra"),
        check_vma=False,
    )
```
